256 devices in a mesh: sp: 32 (over z, y), tp: 4 (over x), dp: 2 (over core).
Axes of the slice: x: 4, y: 4, z: 8, core: 2. Of those that a mesh axis runs over, the one named last changes fastest.
Arguments:
- latent: bfloat16 [2, 32768, 2048], P('dp', 'sp'), may hold values from -4 to 4
- context: bfloat16 [2, 768, 2048], P('dp', 'sp'), may hold values from -6 to 6
- cond: float32 [2, 2048], P('dp'), may hold values from -6 to 6
- ctx_cond: float32 [2048], replicated, may hold values from -6 to 6
- norm_gain: float32 [2048], replicated, may hold values from 0.1 to 1.9
- mod_shift: bfloat16 [2048, 2048], P('sp', 'tp'), may hold values from -0.125 to 0.125
- mod_scale: bfloat16 [2048, 2048], P('sp', 'tp'), may hold values from -0.125 to 0.125
- mod_gate: bfloat16 [2048, 2048], P('sp', 'tp'), may hold values from -0.125 to 0.125
- w_query: bfloat16 [2048, 2048], P(None, 'tp'), may hold values from -0.125 to 0.125
- w_key: bfloat16 [2048, 512], P(None, 'tp'), may hold values from -0.125 to 0.125
- w_value: bfloat16 [2048, 512], P(None, 'tp'), may hold values from -0.125 to 0.125
- w_out: bfloat16 [2048, 2048], P('tp'), may hold values from -2 to 2
- q_gain: float32 [128], replicated, may hold values from 0.1 to 1.9
- k_gain: float32 [128], replicated, may hold values from 0.1 to 1.9
- sinks: float32 [16], P('tp'), may hold values from 3 to 8
Outputs:
- result: bfloat16 [2, 32768, 2048], P('dp', ('sp', 'tp'))
The draws below stay inside these ranges and needn't reach their ends.
All inputs are finite; a program needn't handle non-finite values.
Results may differ from the reference program's by a relative error of at most 0.013.
Values may be sent and summed in bfloat16 or wider, within the bound.
A program may use at most 128 MiB of HBM per device.

```python
import jax
import jax.numpy as jnp
from jax import lax

D = 2048
HEADS = 16
KV_HEADS = 4
HEAD_DIM = 128
WINDOW = 128
GRID_W = 64
CTX = 768
SEQ = 32768
BATCH = 2
N_TP = 4


def block_levels(own_key, shape, shards, least, high):
    level = 1.0
    for axis_at, shards_of in shards:
        heights = jax.random.uniform(jax.random.fold_in(jax.random.fold_in(own_key, 6), axis_at), (shards_of,), jnp.float32, least / len(shards), high / len(shards))
        level = level * jnp.repeat(jnp.exp(heights), shape[axis_at] // shards_of).reshape((-1,) + (1,) * (len(shape) - 1 - axis_at))
    return level


def gaussian(stream_key, extent, deviation, bound, split=(), held_as=jnp.bfloat16):
    values = jax.random.normal(stream_key, extent, jnp.float32) * deviation
    if len(split) > 0:
        values = block_levels(stream_key, extent, split, -0.22, 0.18) * values
    return jnp.clip(values, min=-bound, max=bound).astype(held_as)


def setup_inputs(seed: int = 0) -> dict:
    splits = jax.random.split(jax.random.key(seed), 16)
    latent = gaussian(splits[0], (BATCH, SEQ, D), 0.5, 4.0, ((0, 2), (1, 32)))
    context = gaussian(splits[1], (BATCH, CTX, D), 1.0, 6.0, ((0, 2), (1, 32)))
    cond = gaussian(splits[2], (BATCH, D), 1.0, 6.0, ((0, 2),), jnp.float32)
    ctx_cond = gaussian(splits[3], (D,), 1.0, 6.0, (), jnp.float32)
    norm_gain = jnp.clip(1.0 + 0.18 * jax.random.normal(splits[4], (D,), jnp.float32), 0.1, 1.9)
    mod_shift = gaussian(splits[5], (D, D), D ** -0.5, 0.125, ((0, 32), (1, 4)))
    mod_scale = gaussian(splits[6], (D, D), D ** -0.5, 0.125, ((0, 32), (1, 4)))
    mod_gate = gaussian(splits[7], (D, D), D ** -0.5, 0.125, ((0, 32), (1, 4)))
    w_query = gaussian(splits[8], (D, HEADS * HEAD_DIM), D ** -0.5, 0.125, ((1, 4),))
    w_key = gaussian(splits[9], (D, KV_HEADS * HEAD_DIM), D ** -0.5, 0.125, ((1, 4),))
    w_value = gaussian(splits[10], (D, KV_HEADS * HEAD_DIM), D ** -0.5, 0.125, ((1, 4),))
    w_out = gaussian(splits[11], (HEADS * HEAD_DIM, D), (max(HEADS * HEAD_DIM // 256, 1)) ** -0.5, 2.0, ((0, 4),))
    q_gain = jnp.clip(1.0 + 0.18 * jax.random.normal(splits[12], (HEAD_DIM,), jnp.float32), 0.1, 1.9)
    k_gain = jnp.clip(1.0 + 0.18 * jax.random.normal(splits[13], (HEAD_DIM,), jnp.float32), 0.1, 1.9)
    sinks = jnp.clip(3.0 + 5.0 * jax.random.uniform(splits[14], (HEADS,), jnp.float32) ** block_levels(splits[14], (HEADS,), ((0, 4),), -0.2, 0.2), 3.0, 8.0)
    return dict(latent=latent, context=context, cond=cond, ctx_cond=ctx_cond, norm_gain=norm_gain, mod_shift=mod_shift, mod_scale=mod_scale, mod_gate=mod_gate, w_query=w_query, w_key=w_key, w_value=w_value, w_out=w_out, q_gain=q_gain, k_gain=k_gain, sinks=sinks)


NORM_EPSILON = 1e-06
ROPE_BASE = 10000.0

def head_norm(vectors, gain_row):
    return vectors * lax.rsqrt(lax.optimization_barrier(jnp.mean(vectors * vectors, axis=-1, keepdims=True)) + NORM_EPSILON) * gain_row.astype(jnp.float32)

def modulated(rows_in, gain_row, shift_row, scale_row):
    values = rows_in.astype(jnp.float32)
    normed = values * lax.rsqrt(lax.optimization_barrier(jnp.mean(values * values, axis=-1, keepdims=True)) + NORM_EPSILON) * gain_row.astype(jnp.float32)
    return (normed * (1.0 + scale_row) + shift_row).astype(jnp.bfloat16)

def rotate_half(halves, coords):
    quarter = halves.shape[-1] // 2
    frequency = ROPE_BASE ** (-jnp.arange(quarter, dtype=jnp.float32) / quarter)
    angles = coords.astype(jnp.float32)[:, None] * frequency
    cosine_part = jnp.cos(angles)[:, None, :]
    sine_part = jnp.sin(angles)[:, None, :]
    first_part = halves[..., :quarter]
    second_part = halves[..., quarter:]
    return jnp.concatenate([first_part * cosine_part - second_part * sine_part, second_part * cosine_part + first_part * sine_part], axis=-1)

def rotate(vectors, positions):
    half_dim = vectors.shape[-1] // 2
    return jnp.concatenate([rotate_half(vectors[..., :half_dim], positions // GRID_W), rotate_half(vectors[..., half_dim:], positions % GRID_W)], axis=-1)

def window_attention(lat_queries, lat_keys, lat_values, ctx_keys, ctx_values, sinks):
    seq_len = lat_queries.shape[0]
    group_size = HEADS // KV_HEADS
    score_scale = HEAD_DIM ** (-0.5)
    block_count = seq_len // WINDOW
    query_blocks = lat_queries.reshape(block_count, WINDOW, KV_HEADS, group_size, HEAD_DIM)
    padded_keys = jnp.pad(lat_keys, ((WINDOW, WINDOW), (0, 0), (0, 0)))
    padded_values = jnp.pad(lat_values, ((WINDOW, WINDOW), (0, 0), (0, 0)))
    sink_exp = jnp.exp(sinks.astype(jnp.float32)).reshape(KV_HEADS, group_size)
    key_rows = jnp.arange(3 * WINDOW, dtype=jnp.int32)
    query_rows = jnp.arange(WINDOW, dtype=jnp.int32)
    offset_rows = key_rows[None, :] - query_rows[:, None]
    in_band = (offset_rows >= 0) & (offset_rows <= 2 * WINDOW)
    ctx_key_f = ctx_keys.astype(jnp.float32)
    ctx_value_f = ctx_values.astype(jnp.float32)

    def one_block(inputs):
        block_queries, block_index = inputs
        first_row = (block_index * WINDOW).astype(jnp.int32)
        block_keys = lax.dynamic_slice_in_dim(padded_keys, first_row, 3 * WINDOW, 0).astype(jnp.float32)
        block_values = lax.dynamic_slice_in_dim(padded_values, first_row, 3 * WINDOW, 0).astype(jnp.float32)
        key_pos = first_row - WINDOW + key_rows
        in_window = in_band & ((key_pos >= 0) & (key_pos < seq_len))[None, :]
        block_q = block_queries.astype(jnp.float32)
        scores = jnp.einsum('qhgd,khd->hgqk', block_q, block_keys) * score_scale
        weights = jnp.where(in_window, jnp.exp(scores), 0.0)
        ctx_weights = jnp.exp(jnp.einsum('qhgd,chd->hgqc', block_q, ctx_key_f) * score_scale)
        denominator = lax.optimization_barrier(jnp.sum(weights, axis=-1)) + lax.optimization_barrier(jnp.sum(ctx_weights, axis=-1)) + sink_exp[:, :, None]
        local_probs = (weights / denominator[..., None]).astype(jnp.bfloat16).astype(jnp.float32)
        ctx_probs = (ctx_weights / denominator[..., None]).astype(jnp.bfloat16).astype(jnp.float32)
        block_out = jnp.einsum('hgqk,khd->qhgd', local_probs, block_values) + jnp.einsum('hgqc,chd->qhgd', ctx_probs, ctx_value_f)
        return block_out.astype(jnp.bfloat16).reshape(WINDOW, HEADS * HEAD_DIM)
    attended = lax.map(one_block, (query_blocks, jnp.arange(block_count, dtype=jnp.int32)))
    return attended.reshape(seq_len, HEADS * HEAD_DIM)

def reference(latent, context, cond, ctx_cond, norm_gain, mod_shift, mod_scale, mod_gate, w_query, w_key, w_value, w_out, q_gain, k_gain, sinks):
    seq_len = latent.shape[1]
    ctx_len = context.shape[1]
    group_cols = HEADS * HEAD_DIM // N_TP
    outputs = []
    for sample in range(latent.shape[0]):
        active = jax.nn.silu(jnp.stack([cond[sample].astype(jnp.float32), ctx_cond.astype(jnp.float32)])).astype(jnp.bfloat16)
        shifts = jnp.dot(active, mod_shift, preferred_element_type=jnp.float32)
        scales = jnp.dot(active, mod_scale, preferred_element_type=jnp.float32)
        gate_rows = jnp.dot(active[0:1], mod_gate, preferred_element_type=jnp.float32)
        lat_in = modulated(latent[sample], norm_gain, shifts[0], scales[0])
        ctx_in = modulated(context[sample], norm_gain, shifts[1], scales[1])
        positions = jnp.arange(seq_len, dtype=jnp.int32)
        lat_queries = rotate(head_norm(jnp.dot(lat_in, w_query, preferred_element_type=jnp.float32).reshape(seq_len, HEADS, HEAD_DIM), q_gain), positions).astype(jnp.bfloat16)
        lat_keys = rotate(head_norm(jnp.dot(lat_in, w_key, preferred_element_type=jnp.float32).reshape(seq_len, KV_HEADS, HEAD_DIM), k_gain), positions).astype(jnp.bfloat16)
        lat_values = jnp.dot(lat_in, w_value, preferred_element_type=jnp.float32).astype(jnp.bfloat16).reshape(seq_len, KV_HEADS, HEAD_DIM)
        ctx_keys = head_norm(jnp.dot(ctx_in, w_key, preferred_element_type=jnp.float32).reshape(ctx_len, KV_HEADS, HEAD_DIM), k_gain).astype(jnp.bfloat16)
        ctx_values = jnp.dot(ctx_in, w_value, preferred_element_type=jnp.float32).astype(jnp.bfloat16).reshape(ctx_len, KV_HEADS, HEAD_DIM)
        attended = window_attention(lat_queries, lat_keys, lat_values, ctx_keys, ctx_values, sinks)
        mixed_rows = jnp.zeros((seq_len, D), jnp.float32)
        for group_index in range(N_TP):
            partial_value = jnp.dot(attended[:, group_index * group_cols:(group_index + 1) * group_cols], w_out[group_index * group_cols:(group_index + 1) * group_cols], preferred_element_type=jnp.float32).astype(jnp.bfloat16)
            mixed_rows = mixed_rows + lax.optimization_barrier(partial_value).astype(jnp.float32)
        result = latent[sample].astype(jnp.float32) + gate_rows[0] * mixed_rows
        outputs.append(result.astype(jnp.bfloat16))
    return jnp.stack(outputs)
```

```python
import functools
import math

import jax
import jax.numpy as jnp
import numpy as np
from jax import lax
from jax.experimental import pallas as pl
from jax.experimental.pallas import tpu as pltpu
from jax.sharding import PartitionSpec as P

HEAD_DIM = 128
WINDOW = 128
GRID_W = 64
NORM_EPSILON = 1e-06
ROPE_BASE = 10000.0

MESH = pl.DeviceIdType.MESH
F32 = jnp.float32
BF16 = jnp.bfloat16

NY, NZ, NX = 4, 8, 4
D = 2048
COLS = 512
TOK = 1024
SUB = TOK // NX
ROWS = 256
CROWS = 24
CTX = CROWS * NY * NZ
GROUP = 4
NBLK = TOK // WINDOW
Q_FOLD = HEAD_DIM ** (-0.5) * math.log2(math.e)


def rope_tables(n_sp):
    quarter = HEAD_DIM // 4
    freq = np.float32(ROPE_BASE) ** (-np.arange(quarter, dtype=np.float32) / np.float32(quarter))
    sign = np.concatenate([-np.ones(quarter), np.ones(quarter)]).astype(np.float32)

    def table(coords):
        angles = coords.astype(np.float32)[:, None] * freq[None, :].astype(np.float32)
        angles = np.concatenate([angles, angles], axis=1).astype(np.float64)
        return np.cos(angles).astype(np.float32), np.sin(angles).astype(np.float32) * sign

    row_count = n_sp * TOK // GRID_W
    rc, rs = table(np.arange(row_count))
    cc, cs = table(np.arange(GRID_W))
    rz, cz = np.zeros_like(rc), np.zeros_like(cc)
    rows = np.stack([np.concatenate([rc, rz], 1), np.concatenate([rs, rz], 1)])
    rows = rows.reshape(2, n_sp, TOK // GRID_W, HEAD_DIM).transpose(1, 0, 2, 3)
    cols = np.stack([np.concatenate([cz, cc], 1), np.concatenate([cz, cs], 1)])
    return np.ascontiguousarray(rows), cols


def swap_quarters(v):
    lane = lax.broadcasted_iota(jnp.int32, v.shape, v.ndim - 1)
    even = (lane // 32) % 2 == 0
    return jnp.where(even, pltpu.roll(v, 96, v.ndim - 1), pltpu.roll(v, 32, v.ndim - 1))


def kernel(
    lat_h, ctx_h, cond_h, cctx_h, gain_h, msh_h, msc_h, mga_h, wq_h, wk_h, wv_h, wo_h,
    qg_h, kg_h, sink_h, rowt_h, colt_h, out_h,
    lat, ctx, cnd, gain, modw, wqkv, wo, hg, sink, rowt, colt,
    pm, ym, zs, zm, xm, vec, rinv, lin, cin, tab, qb, kvb, cpiece, cz, ckv, acc, att, attx, res,
    ld, y_s, y_r, z_s, z_r, x_s, x_r, cz_s, cz_r, cy_s, cy_r, h_s, h_r, a_s, a_r,
    s_s, s_r, r_s, r_r, w_s, w_r, d_s, d_r, o_s,
):
    sp = lax.axis_index("sp")
    tp = lax.axis_index("tp")
    dp = lax.axis_index("dp")
    y = lax.rem(sp, NY)
    z = sp // NY
    n_sp = NY * NZ

    def y_peer(d):
        return {"sp": z * NY + lax.rem(y + d, NY)}

    def z_peer(d):
        return {"sp": lax.rem(z + d, NZ) * NY + y}

    def x_peer(d):
        return {"tp": lax.rem(tp + d, NX)}

    partner = {"dp": 1 - dp}
    right = {"sp": lax.rem(sp + 1, n_sp)}
    left = {"sp": lax.rem(sp + n_sp - 1, n_sp)}

    def remote(src, dst, send, recv, dev):
        return pltpu.make_async_remote_copy(
            src_ref=src, dst_ref=dst, send_sem=send, recv_sem=recv, device_id=dev, device_id_type=MESH
        )

    def load(src, dst, k):
        c = pltpu.make_async_copy(src, dst, ld.at[k])
        c.start()
        return c

    barrier = pltpu.get_barrier_semaphore()
    peers = [y_peer(d) for d in range(1, NY)] + [z_peer(d) for d in range(1, NZ)]
    peers += [x_peer(d) for d in range(1, NX)] + [partner, left, right]
    for dev in peers:
        pl.semaphore_signal(barrier, inc=1, device_id=dev, device_id_type=MESH)

    l_mod = [
        load(msh_h, modw.at[0], 0),
        load(msc_h, modw.at[1], 1),
        load(mga_h, modw.at[2], 2),
        load(cond_h, cnd.at[pl.ds(0, 1), :], 3),
        load(cctx_h, cnd.at[pl.ds(1, 1), :], 4),
    ]
    l_lat = [
        load(lat_h.at[pl.ds(i * 256, 256), :], lat.at[pl.ds(i * 256, 256), :], 5 + i) for i in range(4)
    ]
    l_small = [
        load(gain_h, gain, 9),
        load(qg_h, hg.at[pl.ds(0, 1), :], 10),
        load(kg_h, hg.at[pl.ds(1, 1), :], 11),
        load(sink_h, sink, 12),
        load(rowt_h.at[sp], rowt, 13),
        load(colt_h, colt, 14),
        load(ctx_h, ctx, 15),
    ]
    l_kv = [
        load(wk_h, wqkv.at[:, pl.ds(COLS, HEAD_DIM)], 16),
        load(wv_h, wqkv.at[:, pl.ds(COLS + HEAD_DIM, HEAD_DIM)], 17),
    ]
    l_q = load(wq_h, wqkv.at[:, pl.ds(0, COLS)], 18)
    l_wo = load(wo_h, wo.at[pl.ds(pl.multiple_of(tp * COLS, COLS), COLS), :], 19)

    for c in l_mod:
        c.wait()
    half = cnd[:, pl.ds(pl.multiple_of((sp // 2) * 128, 128), 128)]
    act = half / (1.0 + jnp.exp(-half))
    flipped = jnp.concatenate([act[:, 64:], act[:, :64]], axis=1)
    act = jnp.where(lax.rem(sp, 2) == 1, flipped, act)[:, :64].astype(BF16)
    pm[...] = jnp.zeros_like(pm)
    for k in range(3):
        pm[pl.ds(2 * k, 2), :] = jnp.dot(act, modw[k], preferred_element_type=F32)

    pl.semaphore_wait(barrier, len(peers))

    y_cp = [remote(pm, ym.at[d - 1], y_s.at[d - 1], y_r.at[d - 1], y_peer(d)) for d in range(1, NY)]
    for c in y_cp:
        c.start()

    color = lax.rem(y, 2)
    quarter = 2 * color + dp
    other = 2 * (1 - color) + dp
    x_before = lax.rem(tp + 3, NX)
    x_after = lax.rem(tp + 1, NX)
    x_far = lax.rem(tp + 2, NX)

    def wo_rows(block, q, chunk, count):
        return wo.at[pl.ds(pl.multiple_of(block * COLS + q * 128 + chunk * 64, 64), count), :]

    def own_rows(chunk):
        return wo_h.at[pl.ds(pl.multiple_of(quarter * 128 + chunk * 64, 64), 64), :]

    s_cp = [
        [
            remote(own_rows(c), wo_rows(tp, quarter, c, 64), s_s.at[2 * k + c], s_r.at[2 * k + c], x_peer(step))
            for c in range(2)
        ]
        for k, step in enumerate((1, 3))
    ]
    for k in range(2):
        s_cp[k][0].start()

    def norms(i, carry):
        rows = pl.ds(pl.multiple_of(i * 64, 64), 64)
        total = jnp.zeros((64, 128), F32)
        for c in range(D // 128):
            v = lat[rows, pl.ds(c * 128, 128)].astype(F32)
            total = total + v * v
        mean = jnp.sum(total, axis=-1, keepdims=True) * (1.0 / D)
        rinv[rows, :] = jnp.broadcast_to(lax.rsqrt(mean + NORM_EPSILON), (64, 128))
        return carry

    for c in l_lat[:2]:
        c.wait()
    lax.fori_loop(0, 4, norms, 0)

    for c in y_cp:
        c.wait_recv()
    zs[...] = (pm[...] + ym[0]) + (ym[1] + ym[2])
    z_cp = [remote(zs, zm.at[d - 1], z_s.at[d - 1], z_r.at[d - 1], z_peer(d)) for d in range(1, NZ)]
    for c in z_cp:
        c.start()

    for c in l_lat[2:]:
        c.wait()
    lax.fori_loop(4, 16, norms, 0)

    for c in z_cp:
        c.wait_recv()
    xm[tp] = (zs[...] + zm[0]) + (zm[1] + zm[2]) + ((zm[3] + zm[4]) + (zm[5] + zm[6]))
    x_cp = [remote(xm.at[tp], xm.at[tp], x_s.at[d - 1], x_r.at[d - 1], x_peer(d)) for d in range(1, NX)]
    for c in x_cp:
        c.start()
    for k in range(2):
        s_cp[k][1].start()

    for c in l_small + l_kv:
        c.wait()
    c_total = jnp.zeros((CROWS, 128), F32)
    for c in range(D // 128):
        v = ctx[:, pl.ds(c * 128, 128)].astype(F32)
        c_total = c_total + v * v
    c_mean = jnp.sum(c_total, axis=-1, keepdims=True) * (1.0 / D)
    c_inv = jnp.broadcast_to(lax.rsqrt(c_mean + NORM_EPSILON), (CROWS, 128))

    for d in range(1, NX):
        remote(
            xm.at[tp], xm.at[lax.rem(tp + NX - d, NX)], x_s.at[d - 1], x_r.at[d - 1], x_peer(d)
        ).wait_recv()
    for j in range(NX):
        cols = pl.ds(j * COLS, COLS)
        g = gain[:, cols]
        for k, row in ((0, g * (1.0 + xm[j, 2:3, :])), (1, xm[j, 0:1, :]), (2, g * (1.0 + xm[j, 3:4, :])),
                       (3, xm[j, 1:2, :]), (4, xm[j, 4:5, :])):
            vec[k, :, cols] = jnp.broadcast_to(row, (8, COLS))

    for c in range(D // 128):
        cols = pl.ds(c * 128, 128)
        v = ctx[:, cols].astype(F32) * c_inv
        v = v.reshape(CROWS // 8, 8, 128) * vec[2, :, cols][None] + vec[3, :, cols][None]
        cin[:, cols] = v.reshape(CROWS, 128).astype(BF16)
    kv = jnp.dot(cin[...], wqkv[:, pl.ds(COLS, 2 * HEAD_DIM)], preferred_element_type=F32)
    key = kv[:, :HEAD_DIM]
    mean = jnp.mean(key * key, axis=-1, keepdims=True)
    key = key * lax.rsqrt(mean + NORM_EPSILON) * hg[1:2, :]
    cpiece[:, pl.ds(0, HEAD_DIM)] = key.astype(BF16)
    cpiece[:, pl.ds(HEAD_DIM, HEAD_DIM)] = kv[:, HEAD_DIM:].astype(BF16)
    cz_cp = [
        remote(cpiece, cz.at[d - 1], cz_s.at[d - 1], cz_r.at[d - 1], z_peer(d)) for d in range(1, NZ)
    ]
    for c in cz_cp:
        c.start()

    l_q.wait()
    q_gain = jnp.broadcast_to(hg[0:1, :], (8, 128)) * Q_FOLD
    k_gain = jnp.broadcast_to(hg[1:2, :], (8, 128))
    q_swap, k_swap = swap_quarters(q_gain), swap_quarters(k_gain)
    halo_to_left = remote(
        kvb.at[pl.ds(WINDOW, WINDOW), :], kvb.at[pl.ds(TOK + WINDOW, WINDOW), :], h_s.at[0], h_r.at[0], left
    )
    halo_to_right = remote(
        kvb.at[pl.ds(TOK, WINDOW), :], kvb.at[pl.ds(0, WINDOW), :], h_s.at[1], h_r.at[1], right
    )

    def project(i, carry):
        b = lax.rem(3 * i, 4)
        base = pl.multiple_of(b * ROWS, ROWS)

        def modulate(r, c2):
            rows = pl.ds(pl.multiple_of(base + r * 64, 64), 64)
            inv = rinv[rows, :]
            for c in range(D // 128):
                cols = pl.ds(c * 128, 128)
                v = lat[rows, cols].astype(F32) * inv
                v = v.reshape(8, 8, 128) * vec[0, :, cols][None] + vec[1, :, cols][None]
                lin[pl.ds(pl.multiple_of(r * 64, 64), 64), cols] = v.reshape(64, 128).astype(BF16)
            return c2

        lax.fori_loop(0, ROWS // 64, modulate, 0)

        for g in range(ROWS // GRID_W):
            at = pl.ds(g * GRID_W, GRID_W)
            row = b * (ROWS // GRID_W) + g
            cosine = colt[0].reshape(8, 8, 128) + rowt[0, pl.ds(row, 1), :][None]
            sine = colt[1].reshape(8, 8, 128) + rowt[1, pl.ds(row, 1), :][None]
            tab[0, at, :] = (cosine * q_gain[None]).reshape(64, 128)
            tab[1, at, :] = (sine * q_swap[None]).reshape(64, 128)
            tab[2, at, :] = (cosine * k_gain[None]).reshape(64, 128)
            tab[3, at, :] = (sine * k_swap[None]).reshape(64, 128)

        def turned(v, t):
            inv = lax.rsqrt(jnp.mean(v * v, axis=-1, keepdims=True) + NORM_EPSILON)
            return ((v * tab[t] + swap_quarters(v) * tab[t + 1]) * inv).astype(BF16)

        for n in range(3):
            out = jnp.dot(lin[...], wqkv[:, pl.ds(n * 256, 256)], preferred_element_type=F32)
            first, second = out[:, :128], out[:, 128:]
            if n < 2:
                for h, v in ((2 * n, first), (2 * n + 1, second)):
                    t = turned(v, 0)
                    qb[2 * b, pl.ds(h * 128, 128), :] = t[:128]
                    qb[2 * b + 1, pl.ds(h * 128, 128), :] = t[128:]
            else:
                rows = pl.ds(pl.multiple_of(WINDOW + base, 128), ROWS)
                kvb[rows, pl.ds(0, 128)] = turned(first, 2)
                kvb[rows, pl.ds(128, 128)] = second.astype(BF16)

        @pl.when(i == 1)
        def _():
            halo_to_left.start()
            halo_to_right.start()

        return carry

    lax.fori_loop(0, TOK // ROWS, project, 0)

    def to_y(n, block):
        return [
            remote(
                wo_rows(block, quarter, c, 64), wo_rows(block, quarter, c, 64),
                w_s.at[2 * n + c], w_r.at[2 * n + c], y_peer((1, 3)[c]),
            )
            for c in range(2)
        ]

    def from_y(n, block):
        return [
            remote(
                wo_rows(block, other, c, 64), wo_rows(block, other, c, 64),
                w_s.at[2 * n + c], w_r.at[2 * n + c], y_peer((1, 3)[c]),
            )
            for c in range(2)
        ]

    def to_partner(n, block, q):
        rows = wo_rows(block, q, 0, 128)
        return remote(rows, rows, d_s.at[n], d_r.at[n], partner)

    for k, block in enumerate((x_before, x_after)):
        for c in range(2):
            remote(
                own_rows(c), wo_rows(block, quarter, c, 64), s_s.at[2 * k + c], s_r.at[2 * k + c],
                x_peer((1, 3)[k]),
            ).wait_recv()
    r_cp = [
        remote(
            wo_rows(block, quarter, k, 64), wo_rows(block, quarter, k, 64), r_s.at[k], r_r.at[k],
            x_peer((1, 3)[k]),
        )
        for k, block in enumerate((x_before, x_after))
    ]
    for c in r_cp:
        c.start()
    y_w = [to_y(n, block) for n, block in enumerate((x_before, x_after))]
    d_w = [to_partner(n, block, quarter) for n, block in enumerate((x_before, x_after))]
    for n in range(2):
        for c in y_w[n]:
            c.start()
        d_w[n].start()

    for c in cz_cp:
        c.wait_recv()
    pieces = [cpiece[...].astype(F32)] + [cz[d].astype(F32) for d in range(NZ - 1)]
    ckv[pl.ds(0, CROWS * NZ), :] = jnp.concatenate(pieces, axis=0).astype(BF16)
    zrows = CROWS * NZ
    cy_cp = [
        remote(
            ckv.at[pl.ds(0, zrows), :], ckv.at[pl.ds(d * zrows, zrows), :], cy_s.at[d - 1], cy_r.at[d - 1],
            y_peer(d),
        )
        for d in range(1, NY)
    ]
    for c in cy_cp:
        c.start()

    halo_to_left.wait_recv()
    halo_to_right.wait_recv()
    stacked = GROUP * WINDOW
    q_row = lax.rem(lax.broadcasted_iota(jnp.int32, (stacked, WINDOW), 0), WINDOW)
    k_row = lax.broadcasted_iota(jnp.int32, (stacked, WINDOW), 1)
    ahead = k_row - q_row

    def window(i, carry):
        b = lax.rem(i + 1, NBLK)
        rows = pl.ds(pl.multiple_of(b * WINDOW, WINDOW), 3 * WINDOW)
        k = kvb[rows, pl.ds(0, 128)]
        v = kvb[rows, pl.ds(128, 128)]
        s = lax.dot_general(qb[b], k, (((1,), (1,)), ((), ())), preferred_element_type=F32)
        e = jnp.exp2(s)
        no_left = jnp.logical_and(sp == 0, b == 0).astype(jnp.int32) * (2 * WINDOW)
        no_right = jnp.logical_and(sp == n_sp - 1, b == NBLK - 1).astype(jnp.int32) * (2 * WINDOW)
        e_left = jnp.where(ahead >= no_left, e[:, :WINDOW], 0.0)
        e_right = jnp.where(ahead <= -no_right, e[:, 2 * WINDOW :], 0.0)
        p = jnp.concatenate([e_left, e[:, WINDOW : 2 * WINDOW], e_right], axis=1).astype(BF16)
        v2 = jnp.concatenate([v, jnp.ones((3 * WINDOW, 128), BF16)], axis=1)
        acc[b] = jnp.dot(p, v2, preferred_element_type=F32)
        return carry

    lax.fori_loop(0, NBLK, window, 0)

    for k in range(2):
        remote(
            wo_rows(x_far, quarter, k, 64), wo_rows(x_far, quarter, k, 64), r_s.at[k], r_r.at[k],
            x_peer((1, 3)[k]),
        ).wait_recv()
    y_w.append(to_y(2, x_far))
    d_w.append(to_partner(2, x_far, quarter))
    for c in y_w[2]:
        c.start()
    d_w[2].start()

    for c in cy_cp:
        c.wait_recv()

    def att_rows(i):
        return pl.ds(pl.multiple_of(lax.rem(i, 2) * WINDOW, WINDOW), WINDOW)

    my_cols = pl.ds(pl.multiple_of(tp * COLS, COLS), COLS)

    def context_part(i, carry):
        dist = lax.rem(i // 2 + 1, NX)
        dest = lax.rem(tp + dist, NX)
        b = 2 * dest + lax.rem(i, 2)
        k = ckv[:, pl.ds(0, 128)]
        v = ckv[:, pl.ds(128, 128)]
        s = lax.dot_general(qb[b], k, (((1,), (1,)), ((), ())), preferred_element_type=F32)
        p = jnp.exp2(s).astype(BF16)
        v2 = jnp.concatenate([v, jnp.ones((CTX, 128), BF16)], axis=1)
        o = acc[b] + jnp.dot(p, v2, preferred_element_type=F32)
        for h in range(GROUP):
            at = slice(h * WINDOW, (h + 1) * WINDOW)
            sink_exp = jnp.broadcast_to(jnp.exp(sink[:, h : h + 1]), (WINDOW, 128))
            att[i, :, pl.ds(h * 128, 128)] = (o[at, :128] / (o[at, 128:] + sink_exp)).astype(BF16)

        @pl.when(i < 6)
        def _():
            remote(att.at[i], attx.at[att_rows(i), my_cols], a_s.at[i], a_r.at[i], {"tp": dest}).start()

        @pl.when(i >= 6)
        def _():
            attx[att_rows(i), my_cols] = att[i]

        return carry

    lax.fori_loop(0, NBLK, context_part, 0)

    for n, block in enumerate((x_before, x_after, x_far)):
        for c in from_y(n, block):
            c.wait_recv()
    d2_w = [to_partner(3 + n, block, other) for n, block in enumerate((x_before, x_after, x_far))]
    for c in d2_w:
        c.start()

    a_cp = []
    for i in range(6):
        dist = i // 2 + 1
        src = lax.rem(tp + NX - dist, NX)
        cols = pl.ds(pl.multiple_of(src * COLS, COLS), COLS)
        c = remote(
            att.at[i], attx.at[pl.ds((i % 2) * WINDOW, WINDOW), cols], a_s.at[i], a_r.at[i],
            {"tp": lax.rem(tp + dist, NX)},
        )
        c.wait_recv()
        a_cp.append(c)
    p_quarter, p_other = 2 * color + 1 - dp, 2 * (1 - color) + 1 - dp
    for n, block in enumerate((x_before, x_after, x_far)):
        to_partner(n, block, p_quarter).wait_recv()
        to_partner(3 + n, block, p_other).wait_recv()
    l_wo.wait()

    def out_part(n, carry):
        cols = pl.ds(pl.multiple_of(n * 512, 512), 512)
        mixed = jnp.dot(attx[...], wo[:, cols], preferred_element_type=F32)
        own = lat[pl.ds(pl.multiple_of(tp * SUB, SUB), SUB), cols].astype(F32)
        mixed = mixed.reshape(SUB // 8, 8, 512) * vec[4, :, cols][None]
        res[:, cols] = (own + mixed.reshape(SUB, 512)).astype(BF16)
        pltpu.make_async_copy(res.at[:, cols], out_h.at[:, cols], o_s.at[n]).start()
        return carry

    lax.fori_loop(0, D // 512, out_part, 0)

    for c in y_cp + z_cp + x_cp + cz_cp + cy_cp + r_cp + d_w + d2_w + a_cp:
        c.wait_send()
    for group in s_cp + y_w:
        for c in group:
            c.wait_send()
    halo_to_left.wait_send()
    halo_to_right.wait_send()
    for n in range(D // 512):
        cols = pl.ds(n * 512, 512)
        pltpu.make_async_copy(res.at[:, cols], out_h.at[:, cols], o_s.at[n]).wait()


def per_device(*args):
    (latent, context, cond, ctx_cond, norm_gain, mod_shift, mod_scale, mod_gate, w_query, w_key, w_value, w_out,
     q_gain, k_gain, sinks) = args
    rows, cols = rope_tables(NY * NZ)
    operands = (
        latent[0], context[0], cond, ctx_cond.reshape(1, D), norm_gain.reshape(1, D), mod_shift, mod_scale,
        mod_gate, w_query, w_key, w_value, w_out, q_gain.reshape(1, HEAD_DIM), k_gain.reshape(1, HEAD_DIM),
        sinks.reshape(1, GROUP), jnp.asarray(rows), jnp.asarray(cols),
    )
    dma = pltpu.SemaphoreType.DMA
    vm = pltpu.VMEM
    scratch = [
        vm((TOK, D), BF16), vm((CROWS, D), BF16), vm((2, D), F32), vm((1, D), F32), vm((3, 64, COLS), BF16),
        vm((D, COLS + 2 * HEAD_DIM), BF16), vm((D, D), BF16), vm((2, HEAD_DIM), F32), vm((1, GROUP), F32),
        vm((2, TOK // GRID_W, HEAD_DIM), F32), vm((2, GRID_W, HEAD_DIM), F32),
        vm((8, COLS), F32), vm((3, 8, COLS), F32), vm((8, COLS), F32), vm((7, 8, COLS), F32),
        vm((NX, 8, COLS), F32), vm((5, 8, D), F32), vm((TOK, 128), F32), vm((ROWS, D), BF16), vm((CROWS, D), BF16),
        vm((4, ROWS, 128), F32), vm((NBLK, GROUP * WINDOW, 128), BF16), vm((TOK + 2 * WINDOW, 256), BF16),
        vm((CROWS, 256), BF16), vm((NZ - 1, CROWS, 256), BF16), vm((CTX, 256), BF16),
        vm((NBLK, GROUP * WINDOW, 256), F32), vm((NBLK, WINDOW, COLS), BF16), vm((SUB, D), BF16), vm((SUB, D), BF16),
        dma((20,)), dma((3,)), dma((3,)), dma((7,)), dma((7,)), dma((3,)), dma((3,)), dma((7,)), dma((7,)),
        dma((3,)), dma((3,)), dma((2,)), dma((2,)), dma((6,)), dma((6,)),
        dma((4,)), dma((4,)), dma((2,)), dma((2,)), dma((6,)), dma((6,)), dma((6,)), dma((6,)), dma((4,)),
    ]
    result = pl.pallas_call(
        kernel,
        out_shape=jax.ShapeDtypeStruct((SUB, D), BF16),
        in_specs=[pl.BlockSpec(memory_space=pl.ANY)] * len(operands),
        out_specs=pl.BlockSpec(memory_space=pl.ANY),
        scratch_shapes=scratch,
        compiler_params=pltpu.CompilerParams(
            collective_id=0, has_side_effects=True, vmem_limit_bytes=60 * 1024 * 1024
        ),
    )(*operands)
    return result[None]


def solution(mesh):
    in_specs = (
        P("dp", "sp", None), P("dp", "sp", None), P("dp", None), P(), P(), P("sp", "tp"), P("sp", "tp"),
        P("sp", "tp"), P(None, "tp"), P(None, "tp"), P(None, "tp"), P("tp", None), P(), P(), P("tp"),
    )
    out_specs = P("dp", ("sp", "tp"), None)
    return jax.shard_map(per_device, mesh=mesh, in_specs=in_specs, out_specs=out_specs, check_vma=False)
```

```python
import functools
import math

import jax
import jax.numpy as jnp
import numpy as np
from jax import lax
from jax.experimental import pallas as pl
from jax.experimental.pallas import tpu as pltpu
from jax.sharding import PartitionSpec as P

HEAD_DIM = 128
WINDOW = 128
GRID_W = 64
NORM_EPSILON = 1e-06
ROPE_BASE = 10000.0

MESH = pl.DeviceIdType.MESH
F32 = jnp.float32
BF16 = jnp.bfloat16

NY, NZ, NX = 4, 8, 4
D = 2048
COLS = 512
TOK = 1024
SUB = TOK // NX
ROWS = 256
CROWS = 24
CTX = CROWS * NY * NZ
GROUP = 4
NBLK = TOK // WINDOW
Q_FOLD = HEAD_DIM ** (-0.5) * math.log2(math.e)


def rope_tables(n_sp):
    quarter = HEAD_DIM // 4
    freq = np.float32(ROPE_BASE) ** (-np.arange(quarter, dtype=np.float32) / np.float32(quarter))
    sign = np.concatenate([-np.ones(quarter), np.ones(quarter)]).astype(np.float32)

    def table(coords):
        angles = coords.astype(np.float32)[:, None] * freq[None, :].astype(np.float32)
        angles = np.concatenate([angles, angles], axis=1).astype(np.float64)
        return np.cos(angles).astype(np.float32), np.sin(angles).astype(np.float32) * sign

    row_count = n_sp * TOK // GRID_W
    rc, rs = table(np.arange(row_count))
    cc, cs = table(np.arange(GRID_W))
    rz, cz = np.zeros_like(rc), np.zeros_like(cc)
    rows = np.stack([np.concatenate([rc, rz], 1), np.concatenate([rs, rz], 1)])
    rows = rows.reshape(2, n_sp, TOK // GRID_W, HEAD_DIM).transpose(1, 0, 2, 3)
    cols = np.stack([np.concatenate([cz, cc], 1), np.concatenate([cz, cs], 1)])
    return np.ascontiguousarray(rows), cols


def swap_quarters(v):
    lane = lax.broadcasted_iota(jnp.int32, v.shape, v.ndim - 1)
    even = (lane // 32) % 2 == 0
    return jnp.where(even, pltpu.roll(v, 96, v.ndim - 1), pltpu.roll(v, 32, v.ndim - 1))


def kernel(
    lat_h, ctx_h, cond_h, cctx_h, gain_h, msh_h, msc_h, mga_h, wq_h, wk_h, wv_h, wo_h,
    qg_h, kg_h, sink_h, rowt_h, colt_h, out_h,
    lat, ctx, cnd, gain, modw, wqkv, wo, hg, sink, rowt, colt,
    pm, ym, zs, zm, xm, vec, rinv, lin_a, lin_b, cin, tab, qb, kvb, cpiece, cz, ckv, acc, att, attx, mix, res,
    ld, y_s, y_r, z_s, z_r, x_s, x_r, cz_s, cz_r, cy_s, cy_r, h_s, h_r, a_s, a_r,
    s_s, s_r, r_s, r_r, w_s, w_r, d_s, d_r, o_s,
):
    sp = lax.axis_index("sp")
    tp = lax.axis_index("tp")
    dp = lax.axis_index("dp")
    y = lax.rem(sp, NY)
    z = sp // NY
    n_sp = NY * NZ

    def y_peer(d):
        return {"sp": z * NY + lax.rem(y + d, NY)}

    def z_peer(d):
        return {"sp": lax.rem(z + d, NZ) * NY + y}

    def x_peer(d):
        return {"tp": lax.rem(tp + d, NX)}

    partner = {"dp": 1 - dp}
    right = {"sp": lax.rem(sp + 1, n_sp)}
    left = {"sp": lax.rem(sp + n_sp - 1, n_sp)}

    def remote(src, dst, send, recv, dev):
        return pltpu.make_async_remote_copy(
            src_ref=src, dst_ref=dst, send_sem=send, recv_sem=recv, device_id=dev, device_id_type=MESH
        )

    def load(src, dst, k):
        c = pltpu.make_async_copy(src, dst, ld.at[k])
        c.start()
        return c

    barrier = pltpu.get_barrier_semaphore()
    peers = [y_peer(d) for d in range(1, NY)] + [z_peer(d) for d in range(1, NZ)]
    peers += [x_peer(d) for d in range(1, NX)] + [partner, left, right]
    for dev in peers:
        pl.semaphore_signal(barrier, inc=1, device_id=dev, device_id_type=MESH)

    l_mod = [
        load(msh_h, modw.at[0], 0),
        load(msc_h, modw.at[1], 1),
        load(mga_h, modw.at[2], 2),
        load(cond_h, cnd.at[pl.ds(0, 1), :], 3),
        load(cctx_h, cnd.at[pl.ds(1, 1), :], 4),
    ]
    l_lat = [
        load(lat_h.at[pl.ds(i * 256, 256), :], lat.at[pl.ds(i * 256, 256), :], 5 + i) for i in range(4)
    ]
    l_small = [
        load(gain_h, gain, 9),
        load(qg_h, hg.at[pl.ds(0, 1), :], 10),
        load(kg_h, hg.at[pl.ds(1, 1), :], 11),
        load(sink_h, sink, 12),
        load(rowt_h.at[sp], rowt, 13),
        load(colt_h, colt, 14),
        load(ctx_h, ctx, 15),
    ]
    l_kv = [
        load(wk_h, wqkv.at[:, pl.ds(COLS, HEAD_DIM)], 16),
        load(wv_h, wqkv.at[:, pl.ds(COLS + HEAD_DIM, HEAD_DIM)], 17),
    ]
    l_q = load(wq_h, wqkv.at[:, pl.ds(0, COLS)], 18)
    l_wo = load(wo_h, wo.at[pl.ds(pl.multiple_of(tp * COLS, COLS), COLS), :], 19)

    for c in l_mod:
        c.wait()
    half = cnd[:, pl.ds(pl.multiple_of((sp // 2) * 128, 128), 128)]
    act = half / (1.0 + jnp.exp(-half))
    flipped = jnp.concatenate([act[:, 64:], act[:, :64]], axis=1)
    act = jnp.where(lax.rem(sp, 2) == 1, flipped, act)[:, :64].astype(BF16)
    part = jnp.concatenate(
        [jnp.dot(act, modw[k], preferred_element_type=F32) for k in range(3)] + [jnp.zeros((2, COLS), F32)], axis=0
    )
    pm[...] = part.astype(BF16)

    pl.semaphore_wait(barrier, len(peers))

    y_cp = [remote(pm, ym.at[d - 1], y_s.at[d - 1], y_r.at[d - 1], y_peer(d)) for d in range(1, NY)]
    for c in y_cp:
        c.start()

    color = lax.rem(y + z, 2)
    quarter = 2 * color + dp
    other = 2 * (1 - color) + dp
    x_before = lax.rem(tp + 3, NX)
    x_after = lax.rem(tp + 1, NX)
    x_far = lax.rem(tp + 2, NX)

    def wo_rows(block, q, chunk, count, extra=0):
        return wo.at[pl.ds(pl.multiple_of(block * COLS + q * 128 + chunk * 64 + extra, 32), count), :]

    def own_rows(chunk):
        return wo_h.at[pl.ds(pl.multiple_of(quarter * 128 + chunk * 64, 64), 64), :]

    s_cp = [
        [
            remote(own_rows(c), wo_rows(tp, quarter, c, 64), s_s.at[2 * k + c], s_r.at[2 * k + c], x_peer(step))
            for c in range(2)
        ]
        for k, step in enumerate((1, 3))
    ]
    for k in range(2):
        s_cp[k][0].start()

    def norms(i, carry):
        rows = pl.ds(pl.multiple_of(i * 64, 64), 64)
        total = jnp.zeros((64, 128), F32)
        for c in range(D // 128):
            v = lat[rows, pl.ds(c * 128, 128)].astype(F32)
            total = total + v * v
        mean = jnp.sum(total, axis=-1, keepdims=True) * (1.0 / D)
        rinv[rows, :] = jnp.broadcast_to(lax.rsqrt(mean + NORM_EPSILON), (64, 128))
        return carry

    for c in l_lat[:2]:
        c.wait()
    lax.fori_loop(0, 4, norms, 0)

    for c in y_cp:
        c.wait_recv()
    part = (part + ym[0].astype(F32)) + (ym[1].astype(F32) + ym[2].astype(F32))
    zs[...] = part.astype(BF16)
    z_cp = [remote(zs, zm.at[d - 1], z_s.at[d - 1], z_r.at[d - 1], z_peer(d)) for d in range(1, NZ)]
    for c in z_cp:
        c.start()

    for c in l_lat[2:]:
        c.wait()
    lax.fori_loop(4, 16, norms, 0)

    for c in z_cp:
        c.wait_recv()
    for d in range(NZ - 1):
        part = part + zm[d].astype(F32)
    xm[tp] = part
    x_cp = [remote(xm.at[tp], xm.at[tp], x_s.at[d - 1], x_r.at[d - 1], x_peer(d)) for d in range(1, NX)]
    for c in x_cp:
        c.start()
    for k in range(2):
        s_cp[k][1].start()

    for c in l_small + l_kv:
        c.wait()
    c_total = jnp.zeros((CROWS, 128), F32)
    for c in range(D // 128):
        v = ctx[:, pl.ds(c * 128, 128)].astype(F32)
        c_total = c_total + v * v
    c_mean = jnp.sum(c_total, axis=-1, keepdims=True) * (1.0 / D)
    c_inv = jnp.broadcast_to(lax.rsqrt(c_mean + NORM_EPSILON), (CROWS, 128))

    for d in range(1, NX):
        remote(
            xm.at[tp], xm.at[lax.rem(tp + NX - d, NX)], x_s.at[d - 1], x_r.at[d - 1], x_peer(d)
        ).wait_recv()
    for j in range(NX):
        cols = pl.ds(j * COLS, COLS)
        g = gain[:, cols]
        for k, row in ((0, g * (1.0 + xm[j, 2:3, :])), (1, xm[j, 0:1, :]), (2, g * (1.0 + xm[j, 3:4, :])),
                       (3, xm[j, 1:2, :]), (4, xm[j, 4:5, :])):
            vec[k, :, cols] = jnp.broadcast_to(row, (8, COLS))

    for c in range(D // 128):
        cols = pl.ds(c * 128, 128)
        v = ctx[:, cols].astype(F32) * c_inv
        v = v.reshape(CROWS // 8, 8, 128) * vec[2, :, cols][None] + vec[3, :, cols][None]
        cin[:, cols] = v.reshape(CROWS, 128).astype(BF16)
    kv = jnp.dot(cin[...], wqkv[:, pl.ds(COLS, 2 * HEAD_DIM)], preferred_element_type=F32)
    key = kv[:, :HEAD_DIM]
    mean = jnp.mean(key * key, axis=-1, keepdims=True)
    key = key * lax.rsqrt(mean + NORM_EPSILON) * hg[1:2, :]
    cpiece[:, pl.ds(0, HEAD_DIM)] = key.astype(BF16)
    cpiece[:, pl.ds(HEAD_DIM, HEAD_DIM)] = kv[:, HEAD_DIM:].astype(BF16)
    cz_cp = [
        remote(cpiece, cz.at[d - 1], cz_s.at[d - 1], cz_r.at[d - 1], z_peer(d)) for d in range(1, NZ)
    ]
    for c in cz_cp:
        c.start()

    l_q.wait()
    q_gain = jnp.broadcast_to(hg[0:1, :], (8, 128)) * Q_FOLD
    k_gain = jnp.broadcast_to(hg[1:2, :], (8, 128))
    q_swap, k_swap = swap_quarters(q_gain), swap_quarters(k_gain)
    halo_to_left = remote(
        kvb.at[pl.ds(WINDOW, WINDOW), :], kvb.at[pl.ds(TOK + WINDOW, WINDOW), :], h_s.at[0], h_r.at[0], left
    )
    halo_to_right = remote(
        kvb.at[pl.ds(TOK, WINDOW), :], kvb.at[pl.ds(0, WINDOW), :], h_s.at[1], h_r.at[1], right
    )

    side_peers = (y_peer(1), y_peer(NY - 1), z_peer(1), z_peer(NZ - 1))
    blocks = (x_before, x_after, x_far)

    def to_side(n, k):
        rows = wo_rows(blocks[n], quarter, k // 2, 32, 32 * (k % 2))
        return remote(rows, rows, w_s.at[4 * n + k], w_r.at[4 * n + k], side_peers[k])

    def from_side(n, k):
        rows = wo_rows(blocks[n], other, k // 2, 32, 32 * (k % 2))
        return remote(rows, rows, w_s.at[4 * n + k], w_r.at[4 * n + k], side_peers[k])

    def to_partner(n, block, q):
        rows = wo_rows(block, q, 0, 128)
        return remote(rows, rows, d_s.at[n], d_r.at[n], partner)

    sent = []

    def go(c):
        c.start()
        sent.append(c)

    zrows = CROWS * NZ
    near = 4 * CROWS

    def pass_context(first):
        group = (1, 7, 2) if first else (6, 3, 5, 4)
        for d in group:
            cz_cp[d - 1].wait_recv()
        pieces = [cz[d - 1].astype(F32) for d in group]
        if first:
            pieces = [cpiece[...].astype(F32)] + pieces
        base = 0 if first else near
        ckv[pl.ds(base, near), :] = jnp.concatenate(pieces, axis=0).astype(BF16)
        for d in range(1, NY):
            k = 2 * (d - 1) + (0 if first else 1)
            go(remote(
                ckv.at[pl.ds(base, near), :], ckv.at[pl.ds(d * zrows + base, near), :], cy_s.at[k], cy_r.at[k],
                y_peer(d),
            ))

    def modulate(b, lin, r):
        rows = pl.ds(b * ROWS + r * 64, 64)
        inv = rinv[rows, :]
        for c in range(D // 128):
            cols = pl.ds(c * 128, 128)
            v = lat[rows, cols].astype(F32) * inv
            v = v.reshape(8, 8, 128) * vec[0, :, cols][None] + vec[1, :, cols][None]
            lin[pl.ds(r * 64, 64), cols] = v.reshape(64, 128).astype(BF16)

    def project(b, lin, next_b, next_lin):
        for g in range(ROWS // GRID_W):
            at = pl.ds(g * GRID_W, GRID_W)
            row = b * (ROWS // GRID_W) + g
            cosine = colt[0].reshape(8, 8, 128) + rowt[0, pl.ds(row, 1), :][None]
            sine = colt[1].reshape(8, 8, 128) + rowt[1, pl.ds(row, 1), :][None]
            tab[0, at, :] = (cosine * q_gain[None]).reshape(64, 128)
            tab[1, at, :] = (sine * q_swap[None]).reshape(64, 128)
            tab[2, at, :] = (cosine * k_gain[None]).reshape(64, 128)
            tab[3, at, :] = (sine * k_swap[None]).reshape(64, 128)

        def turned(v, t):
            inv = lax.rsqrt(jnp.mean(v * v, axis=-1, keepdims=True) + NORM_EPSILON)
            return ((v * tab[t] + swap_quarters(v) * tab[t + 1]) * inv).astype(BF16)

        for n in (2, 0, 1):
            out = jnp.dot(lin[...], wqkv[:, pl.ds(n * 256, 256)], preferred_element_type=F32)
            if next_b is not None:
                for r in {2: (0,), 0: (1, 2), 1: (3,)}[n]:
                    modulate(next_b, next_lin, r)
            first, second = out[:, :128], out[:, 128:]
            if n < 2:
                for h, v in ((2 * n, first), (2 * n + 1, second)):
                    t = turned(v, 0)
                    qb[2 * b, pl.ds(h * 128, 128), :] = t[:128]
                    qb[2 * b + 1, pl.ds(h * 128, 128), :] = t[128:]
            else:
                rows = pl.ds(WINDOW + b * ROWS, ROWS)
                kvb[rows, pl.ds(0, 128)] = turned(first, 2)
                kvb[rows, pl.ds(128, 128)] = second.astype(BF16)

    for r in range(ROWS // 64):
        modulate(0, lin_a, r)
    project(0, lin_a, 3, lin_b)
    project(3, lin_b, 1, lin_a)
    halo_to_left.start()
    halo_to_right.start()
    pass_context(True)
    for k, block in enumerate((x_before, x_after)):
        for c in range(2):
            remote(
                own_rows(c), wo_rows(block, quarter, c, 64), s_s.at[2 * k + c], s_r.at[2 * k + c],
                x_peer((1, 3)[k]),
            ).wait_recv()
    for k, block in enumerate((x_before, x_after)):
        rows = wo_rows(block, quarter, k, 64)
        go(remote(rows, rows, r_s.at[k], r_r.at[k], x_peer((1, 3)[k])))
    for n in range(2):
        go(to_side(n, 2))
        go(to_side(n, 3))
        go(to_partner(n, blocks[n], quarter))
    project(1, lin_a, 2, lin_b)
    pass_context(False)
    for n in range(2):
        go(to_side(n, 0))
        go(to_side(n, 1))
    project(2, lin_b, None, None)

    halo_to_left.wait_recv()
    halo_to_right.wait_recv()
    stacked = GROUP * WINDOW
    q_row = lax.rem(lax.broadcasted_iota(jnp.int32, (stacked, WINDOW), 0), WINDOW)
    k_row = lax.broadcasted_iota(jnp.int32, (stacked, WINDOW), 1)
    ahead = k_row - q_row

    def window(b):
        rows = pl.ds(pl.multiple_of(b * WINDOW, WINDOW), 3 * WINDOW)
        k = kvb[rows, pl.ds(0, 128)]
        v = kvb[rows, pl.ds(128, 128)]
        s = lax.dot_general(qb[b], k, (((1,), (1,)), ((), ())), preferred_element_type=F32)
        e = jnp.exp2(s)
        no_left = jnp.logical_and(sp == 0, b == 0).astype(jnp.int32) * (2 * WINDOW)
        no_right = jnp.logical_and(sp == n_sp - 1, b == NBLK - 1).astype(jnp.int32) * (2 * WINDOW)
        e_left = jnp.where(ahead >= no_left, e[:, :WINDOW], 0.0)
        e_right = jnp.where(ahead <= -no_right, e[:, 2 * WINDOW :], 0.0)
        p = jnp.concatenate([e_left, e[:, WINDOW : 2 * WINDOW], e_right], axis=1).astype(BF16)
        v2 = jnp.concatenate([v, jnp.ones((3 * WINDOW, 128), BF16)], axis=1)
        return jnp.dot(p, v2, preferred_element_type=F32)

    def window_pair(i, carry):
        b0 = 2 * i + 1
        b1 = lax.rem(2 * i + 2, NBLK)
        o0, o1 = window(b0), window(b1)
        acc[b0] = o0
        acc[b1] = o1
        return carry

    lax.fori_loop(0, NBLK // 2, window_pair, 0)

    for k in range(2):
        remote(
            wo_rows(x_far, quarter, k, 64), wo_rows(x_far, quarter, k, 64), r_s.at[k], r_r.at[k],
            x_peer((1, 3)[k]),
        ).wait_recv()
    for k in range(4):
        go(to_side(2, k))
    go(to_partner(2, x_far, quarter))

    for d in range(1, NY):
        for f in range(2):
            part_rows = pl.ds(d * zrows + f * near, near)
            remote(
                ckv.at[pl.ds(f * near, near), :], ckv.at[part_rows, :], cy_s.at[2 * (d - 1) + f],
                cy_r.at[2 * (d - 1) + f], y_peer(d),
            ).wait_recv()

    def context_part(b):
        k = ckv[:, pl.ds(0, 128)]
        v = ckv[:, pl.ds(128, 128)]
        s = lax.dot_general(qb[b], k, (((1,), (1,)), ((), ())), preferred_element_type=F32)
        p = jnp.exp2(s).astype(BF16)
        v2 = jnp.concatenate([v, jnp.ones((CTX, 128), BF16)], axis=1)
        return acc[b] + jnp.dot(p, v2, preferred_element_type=F32)

    def finish(o, h):
        at = slice(h * WINDOW, (h + 1) * WINDOW)
        sink_exp = jnp.broadcast_to(jnp.exp(sink[:, h : h + 1]), (WINDOW, 128))
        return (o[at, :128] / (o[at, 128:] + sink_exp)).astype(BF16)

    a_cp = {}

    def pair(members):
        outs = [context_part(2 * lax.rem(tp + dist, NX) + half) for dist, half in members]
        for (dist, half), o in zip(members, outs):
            rows = pl.ds(half * WINDOW, WINDOW)
            for h in range(GROUP):
                cols = pl.ds(h * 128, 128)
                if dist == 0:
                    attx[0, rows, cols] = finish(o, h)
                else:
                    att[dist - 1, rows, cols] = finish(o, h)
            if dist:
                k = 2 * (dist - 1) + half
                c = remote(att.at[dist - 1, rows, :], attx.at[dist, rows, :], a_s.at[k], a_r.at[k], x_peer(dist))
                go(c)
                a_cp[k] = c

    pair(((1, 0), (3, 0)))
    pair(((1, 1), (3, 1)))
    for n in range(2):
        for k in range(4):
            from_side(n, k).wait_recv()
        go(to_partner(3 + n, blocks[n], other))
    pair(((2, 0), (2, 1)))
    pair(((0, 0), (0, 1)))

    def piece(dist, block, cols):
        rows = pl.ds(pl.multiple_of(block * COLS, COLS), COLS)
        return jnp.dot(attx[dist], wo[rows, cols], preferred_element_type=F32)

    l_wo.wait()

    def own_part(n, carry):
        cols = pl.ds(pl.multiple_of(n * 512, 512), 512)
        mix[:, cols] = piece(0, tp, cols)
        return carry

    lax.fori_loop(0, D // 512, own_part, 0)

    for k in range(4):
        from_side(2, k).wait_recv()
    go(to_partner(5, x_far, other))
    p_quarter, p_other = 2 * color + 1 - dp, 2 * (1 - color) + 1 - dp
    for n in range(2):
        to_partner(n, blocks[n], p_quarter).wait_recv()
        to_partner(3 + n, blocks[n], p_other).wait_recv()
    for k in (0, 1, 4, 5):
        a_cp[k].wait_recv()

    def near_part(n, carry):
        cols = pl.ds(pl.multiple_of(n * 512, 512), 512)
        mix[:, cols] = mix[:, cols] + (piece(1, x_before, cols) + piece(3, x_after, cols))
        return carry

    lax.fori_loop(0, D // 512, near_part, 0)

    to_partner(2, x_far, p_quarter).wait_recv()
    to_partner(5, x_far, p_other).wait_recv()
    for k in (2, 3):
        a_cp[k].wait_recv()

    def far_part(n, carry):
        cols = pl.ds(pl.multiple_of(n * 512, 512), 512)
        mixed = mix[:, cols] + piece(2, x_far, cols)
        own = lat[pl.ds(pl.multiple_of(tp * SUB, SUB), SUB), cols].astype(F32)
        mixed = mixed.reshape(SUB // 8, 8, 512) * vec[4, :, cols][None]
        res[:, cols] = (own + mixed.reshape(SUB, 512)).astype(BF16)
        pltpu.make_async_copy(res.at[:, cols], out_h.at[:, cols], o_s.at[n]).start()
        return carry

    lax.fori_loop(0, D // 512, far_part, 0)

    for c in y_cp + z_cp + x_cp + cz_cp + sent:
        c.wait_send()
    for group in s_cp:
        for c in group:
            c.wait_send()
    halo_to_left.wait_send()
    halo_to_right.wait_send()
    for n in range(D // 512):
        cols = pl.ds(n * 512, 512)
        pltpu.make_async_copy(res.at[:, cols], out_h.at[:, cols], o_s.at[n]).wait()


def per_device(*args):
    (latent, context, cond, ctx_cond, norm_gain, mod_shift, mod_scale, mod_gate, w_query, w_key, w_value, w_out,
     q_gain, k_gain, sinks) = args
    rows, cols = rope_tables(NY * NZ)
    operands = (
        latent[0], context[0], cond, ctx_cond.reshape(1, D), norm_gain.reshape(1, D), mod_shift, mod_scale,
        mod_gate, w_query, w_key, w_value, w_out, q_gain.reshape(1, HEAD_DIM), k_gain.reshape(1, HEAD_DIM),
        sinks.reshape(1, GROUP), jnp.asarray(rows), jnp.asarray(cols),
    )
    dma = pltpu.SemaphoreType.DMA
    vm = pltpu.VMEM
    scratch = [
        vm((TOK, D), BF16), vm((CROWS, D), BF16), vm((2, D), F32), vm((1, D), F32), vm((3, 64, COLS), BF16),
        vm((D, COLS + 2 * HEAD_DIM), BF16), vm((D, D), BF16), vm((2, HEAD_DIM), F32), vm((1, GROUP), F32),
        vm((2, TOK // GRID_W, HEAD_DIM), F32), vm((2, GRID_W, HEAD_DIM), F32),
        vm((8, COLS), BF16), vm((3, 8, COLS), BF16), vm((8, COLS), BF16), vm((7, 8, COLS), BF16),
        vm((NX, 8, COLS), F32), vm((5, 8, D), F32), vm((TOK, 128), F32), vm((ROWS, D), BF16), vm((ROWS, D), BF16),
        vm((CROWS, D), BF16),
        vm((4, ROWS, 128), F32), vm((NBLK, GROUP * WINDOW, 128), BF16), vm((TOK + 2 * WINDOW, 256), BF16),
        vm((CROWS, 256), BF16), vm((NZ - 1, CROWS, 256), BF16), vm((CTX, 256), BF16),
        vm((NBLK, GROUP * WINDOW, 256), F32), vm((NX - 1, SUB, COLS), BF16), vm((NX, SUB, COLS), BF16),
        vm((SUB, D), F32), vm((SUB, D), BF16),
        dma((20,)), dma((3,)), dma((3,)), dma((7,)), dma((7,)), dma((3,)), dma((3,)), dma((7,)), dma((7,)),
        dma((6,)), dma((6,)), dma((2,)), dma((2,)), dma((6,)), dma((6,)),
        dma((4,)), dma((4,)), dma((2,)), dma((2,)), dma((12,)), dma((12,)), dma((6,)), dma((6,)), dma((4,)),
    ]
    result = pl.pallas_call(
        kernel,
        out_shape=jax.ShapeDtypeStruct((SUB, D), BF16),
        in_specs=[pl.BlockSpec(memory_space=pl.ANY)] * len(operands),
        out_specs=pl.BlockSpec(memory_space=pl.ANY),
        scratch_shapes=scratch,
        compiler_params=pltpu.CompilerParams(
            collective_id=0, has_side_effects=True, vmem_limit_bytes=60 * 1024 * 1024
        ),
    )(*operands)
    return result[None]


def solution(mesh):
    in_specs = (
        P("dp", "sp", None), P("dp", "sp", None), P("dp", None), P(), P(), P("sp", "tp"), P("sp", "tp"),
        P("sp", "tp"), P(None, "tp"), P(None, "tp"), P(None, "tp"), P("tp", None), P(), P(), P("tp"),
    )
    out_specs = P("dp", ("sp", "tp"), None)
    return jax.shard_map(per_device, mesh=mesh, in_specs=in_specs, out_specs=out_specs, check_vma=False)
```

```python
import functools
import math

import jax
import jax.numpy as jnp
import numpy as np
from jax import lax
from jax.experimental import pallas as pl
from jax.experimental.pallas import tpu as pltpu
from jax.sharding import PartitionSpec as P

HEAD_DIM = 128
WINDOW = 128
GRID_W = 64
NORM_EPSILON = 1e-06
ROPE_BASE = 10000.0

MESH = pl.DeviceIdType.MESH
F32 = jnp.float32
BF16 = jnp.bfloat16

NY, NZ, NX = 4, 8, 4
D = 2048
COLS = 512
TOK = 1024
SUB = TOK // NX
ROWS = 256
CROWS = 24
CTX = CROWS * NY * NZ
GROUP = 4
NBLK = TOK // WINDOW
Q_FOLD = HEAD_DIM ** (-0.5) * math.log2(math.e)


def rope_tables(n_sp):
    quarter = HEAD_DIM // 4
    freq = np.float32(ROPE_BASE) ** (-np.arange(quarter, dtype=np.float32) / np.float32(quarter))
    sign = np.concatenate([-np.ones(quarter), np.ones(quarter)]).astype(np.float32)

    def table(coords):
        angles = coords.astype(np.float32)[:, None] * freq[None, :].astype(np.float32)
        angles = np.concatenate([angles, angles], axis=1).astype(np.float64)
        return np.cos(angles).astype(np.float32), np.sin(angles).astype(np.float32) * sign

    row_count = n_sp * TOK // GRID_W
    rc, rs = table(np.arange(row_count))
    cc, cs = table(np.arange(GRID_W))
    rz, cz = np.zeros_like(rc), np.zeros_like(cc)
    rows = np.stack([np.concatenate([rc, rz], 1), np.concatenate([rs, rz], 1)])
    rows = rows.reshape(2, n_sp, TOK // GRID_W, HEAD_DIM).transpose(1, 0, 2, 3)
    cols = np.stack([np.concatenate([cz, cc], 1), np.concatenate([cz, cs], 1)])
    return np.ascontiguousarray(rows), cols


def swap_quarters(v):
    lane = lax.broadcasted_iota(jnp.int32, v.shape, v.ndim - 1)
    even = (lane // 32) % 2 == 0
    return jnp.where(even, pltpu.roll(v, 96, v.ndim - 1), pltpu.roll(v, 32, v.ndim - 1))


def kernel(
    lat_h, ctx_h, cond_h, cctx_h, gain_h, msh_h, msc_h, mga_h, wq_h, wk_h, wv_h, wo_h,
    qg_h, kg_h, sink_h, rowt_h, colt_h, out_h,
    lat, ctx, cnd, gain, modw, wqkv, wo, hg, sink, rowt, colt,
    pm, zm, jm, vec, rinv, lin0, lin1, lin2, lin3, cin, tab, qb, kvb, cpiece, cz, ckv, acc, att, attx, mix, res,
    ld, m_s, m_r, c_s, c_r, h_s, h_r, a_s, a_r, w_s, w_r, o_s,
):
    sp = lax.axis_index("sp")
    tp = lax.axis_index("tp")
    dp = lax.axis_index("dp")
    y = lax.rem(sp, NY)
    z = sp // NY
    n_sp = NY * NZ

    def y_peer(d):
        return {"sp": z * NY + lax.rem(y + d, NY)}

    def z_peer(d):
        return {"sp": lax.rem(z + d, NZ) * NY + y}

    def x_peer(d):
        return {"tp": lax.rem(tp + d, NX)}

    def yx_peer(dy, dx):
        return {"sp": z * NY + lax.rem(y + dy, NY), "tp": lax.rem(tp + dx, NX)}

    partner = {"dp": 1 - dp}
    right = {"sp": lax.rem(sp + 1, n_sp)}
    left = {"sp": lax.rem(sp + n_sp - 1, n_sp)}

    def remote(src, dst, send, recv, dev):
        return pltpu.make_async_remote_copy(
            src_ref=src, dst_ref=dst, send_sem=send, recv_sem=recv, device_id=dev, device_id_type=MESH
        )

    def arrived(ref, recv):
        remote(ref, ref, m_s.at[0], recv, partner).wait_recv()

    def left_here(ref, send):
        remote(ref, ref, send, m_r.at[0], partner).wait_send()

    def load(src, dst, k):
        pltpu.make_async_copy(src, dst, ld.at[k]).start()

    def loaded(ref, k):
        pltpu.make_async_copy(ref, ref, ld.at[k]).wait()

    barrier = pltpu.get_barrier_semaphore()
    yx = [(dy, dx) for dx in range(NX) for dy in range(NY) if dy or dx]
    yx.sort(key=lambda p: -(min(p[0], NY - p[0]) + min(p[1], NX - p[1])))
    z_far = sorted(range(1, NZ), key=lambda d: -min(d, NZ - d))
    peers = [yx_peer(dy, dx) for dy, dx in yx] + [z_peer(d) for d in z_far] + [partner, left, right]
    for dev in peers:
        pl.semaphore_signal(barrier, inc=1, device_id=dev, device_id_type=MESH)

    load(msh_h, modw.at[0], 0)
    load(msc_h, modw.at[1], 0)
    load(mga_h, modw.at[2], 0)
    load(cond_h, cnd.at[pl.ds(0, 1), :], 1)
    load(cctx_h, cnd.at[pl.ds(1, 1), :], 1)
    for i in range(4):
        load(lat_h.at[pl.ds(i * 256, 256), :], lat.at[pl.ds(i * 256, 256), :], 2 + i // 2)
    load(qg_h, hg.at[pl.ds(0, 1), :], 4)
    load(kg_h, hg.at[pl.ds(1, 1), :], 4)
    load(rowt_h.at[sp], rowt, 5)
    load(colt_h, colt, 6)
    load(gain_h, gain, 7)
    load(sink_h, sink, 8)
    load(ctx_h, ctx, 9)
    load(wk_h, wqkv.at[:, pl.ds(COLS, HEAD_DIM)], 10)
    load(wv_h, wqkv.at[:, pl.ds(COLS + HEAD_DIM, HEAD_DIM)], 10)
    load(wq_h, wqkv.at[:, pl.ds(0, COLS)], 11)
    own_wo = wo.at[pl.ds(pl.multiple_of(tp * COLS, COLS), COLS), :]
    load(wo_h, own_wo, 12)

    loaded(modw, 0)
    loaded(cnd, 1)
    half = cnd[:, pl.ds(pl.multiple_of((sp // 2) * 128, 128), 128)]
    act = half / (1.0 + jnp.exp(-half))
    flipped = jnp.concatenate([act[:, 64:], act[:, :64]], axis=1)
    act = jnp.where(lax.rem(sp, 2) == 1, flipped, act)[:, :64].astype(BF16)
    part = jnp.concatenate(
        [jnp.dot(act, modw[k], preferred_element_type=F32) for k in range(3)] + [jnp.zeros((2, COLS), F32)], axis=0
    )
    pm[...] = part.astype(BF16)

    pl.semaphore_wait(barrier, len(peers))

    for d in z_far:
        remote(pm, zm.at[d - 1], m_s.at[0], m_r.at[0], z_peer(d)).start()

    color = lax.rem(y + z, 2)
    quarter = 2 * color + dp
    other = 2 * (1 - color) + dp
    x_before = lax.rem(tp + 3, NX)
    x_after = lax.rem(tp + 1, NX)
    x_far = lax.rem(tp + 2, NX)
    blocks = (x_before, x_after, x_far)

    def wo_rows(block, q, first, count):
        return wo.at[pl.ds(pl.multiple_of(block * COLS + q * 128 + first, 16), count), :]

    def send_own(first, count):
        src = wo_h.at[pl.ds(pl.multiple_of(quarter * 128 + first, 16), count), :]
        for step in (1, 3):
            remote(src, wo_rows(tp, quarter, first, count), w_s, w_r.at[0], x_peer(step)).start()

    send_own(0, 48)

    def norms(i, carry):
        rows = pl.ds(pl.multiple_of(i * 64, 64), 64)
        total = jnp.zeros((64, 128), F32)
        for c in range(D // 128):
            v = lat[rows, pl.ds(c * 128, 128)].astype(F32)
            total = total + v * v
        mean = jnp.sum(total, axis=-1, keepdims=True) * (1.0 / D)
        rinv[rows, :] = jnp.broadcast_to(lax.rsqrt(mean + NORM_EPSILON), (64, 128))
        return carry

    loaded(lat.at[pl.ds(0, 512), :], 2)
    lax.fori_loop(0, 8, norms, 0)

    loaded(hg, 4)
    loaded(rowt, 5)
    loaded(colt, 6)
    q_gain = jnp.broadcast_to(hg[0:1, :], (8, 128)) * Q_FOLD
    k_gain = jnp.broadcast_to(hg[1:2, :], (8, 128))
    q_swap, k_swap = swap_quarters(q_gain), swap_quarters(k_gain)

    def tables(row, carry):
        at = pl.ds(pl.multiple_of(row * GRID_W, GRID_W), GRID_W)
        cosine = colt[0].reshape(8, 8, 128) + rowt[0, pl.ds(row, 1), :][None]
        sine = colt[1].reshape(8, 8, 128) + rowt[1, pl.ds(row, 1), :][None]
        tab[0, at, :] = (cosine * q_gain[None]).reshape(64, 128)
        tab[1, at, :] = (sine * q_swap[None]).reshape(64, 128)
        tab[2, at, :] = (cosine * k_gain[None]).reshape(64, 128)
        tab[3, at, :] = (sine * k_swap[None]).reshape(64, 128)
        return carry

    lax.fori_loop(0, TOK // GRID_W, tables, 0)

    arrived(zm, m_r.at[0])
    for d in range(NZ - 1):
        part = part + zm[d].astype(F32)
    jm[0] = part.astype(BF16)
    for dy, dx in yx:
        remote(jm.at[0], jm.at[NY * dx + dy], m_s.at[1], m_r.at[1], yx_peer(dy, dx)).start()
    send_own(48, 80)

    loaded(lat.at[pl.ds(512, 512), :], 3)
    lax.fori_loop(8, 16, norms, 0)

    loaded(ctx, 9)
    c_total = jnp.zeros((CROWS, 128), F32)
    for c in range(D // 128):
        v = ctx[:, pl.ds(c * 128, 128)].astype(F32)
        c_total = c_total + v * v
    c_mean = jnp.sum(c_total, axis=-1, keepdims=True) * (1.0 / D)
    c_inv = jnp.broadcast_to(lax.rsqrt(c_mean + NORM_EPSILON), (CROWS, 128))
    loaded(gain, 7)
    loaded(sink, 8)
    loaded(wqkv.at[:, pl.ds(COLS, 2 * HEAD_DIM)], 10)

    arrived(jm.at[pl.ds(1, NX * NY - 1)], m_r.at[1])
    for dx in range(NX):
        m = part if dx == 0 else jm[NY * dx].astype(F32)
        for dy in range(1, NY):
            m = m + jm[NY * dx + dy].astype(F32)
        cols = pl.ds(pl.multiple_of(lax.rem(tp + NX - dx, NX) * COLS, COLS), COLS)
        g = gain[:, cols]
        for k, row in ((0, g * (1.0 + m[2:3])), (1, m[0:1]), (2, g * (1.0 + m[3:4])), (3, m[1:2]), (4, m[4:5])):
            vec[k, :, cols] = jnp.broadcast_to(row, (8, COLS))

    for c in range(D // 128):
        cols = pl.ds(c * 128, 128)
        v = ctx[:, cols].astype(F32) * c_inv
        v = v.reshape(CROWS // 8, 8, 128) * vec[2, :, cols][None] + vec[3, :, cols][None]
        cin[:, cols] = v.reshape(CROWS, 128).astype(BF16)
    kv = jnp.dot(cin[...], wqkv[:, pl.ds(COLS, 2 * HEAD_DIM)], preferred_element_type=F32)
    key = kv[:, :HEAD_DIM]
    mean = jnp.mean(key * key, axis=-1, keepdims=True)
    key = key * lax.rsqrt(mean + NORM_EPSILON) * hg[1:2, :]
    cpiece[:, pl.ds(0, HEAD_DIM)] = key.astype(BF16)
    cpiece[:, pl.ds(HEAD_DIM, HEAD_DIM)] = kv[:, HEAD_DIM:].astype(BF16)
    near_z, far_z = (1, 7, 2), (4, 5, 3, 6)
    for k, group in ((1, far_z), (0, near_z)):
        for n, d in enumerate(group):
            remote(cpiece, cz.at[3 * k + n], c_s.at[0], c_r.at[k], z_peer(d)).start()

    loaded(wqkv.at[:, pl.ds(0, COLS)], 11)
    side_peers = (y_peer(1), y_peer(NY - 1), z_peer(1), z_peer(NZ - 1))

    def to_side(n, k):
        rows = wo_rows(blocks[n], quarter, 32 * k, 32)
        remote(rows, rows, w_s, w_r.at[2 + n // 2], side_peers[k]).start()

    def to_partner(n, q):
        rows = wo_rows(blocks[n], q, 0, 128)
        remote(rows, rows, w_s, w_r.at[4 + n // 2], partner).start()

    zrows = CROWS * NZ
    near = 4 * CROWS

    def pass_context(first):
        if first:
            arrived(cz.at[pl.ds(0, 3)], c_r.at[0])
            pieces = [cpiece[...].astype(F32)] + [cz[n].astype(F32) for n in range(3)]
        else:
            arrived(cz.at[pl.ds(3, 4)], c_r.at[1])
            pieces = [cz[n].astype(F32) for n in range(3, 7)]
        base = 0 if first else near
        ckv[pl.ds(base, near), :] = jnp.concatenate(pieces, axis=0).astype(BF16)
        for d in (2, 1, 3):
            rows = pl.ds(d * zrows + base, near)
            remote(ckv.at[pl.ds(base, near), :], ckv.at[rows, :], c_s.at[1], c_r.at[2], y_peer(d)).start()

    def modulate(b, lin, r):
        rows = pl.ds(b * ROWS + r * 64, 64)
        inv = rinv[rows, :]
        for c in range(D // 128):
            cols = pl.ds(c * 128, 128)
            v = lat[rows, cols].astype(F32) * inv
            v = v.reshape(8, 8, 128) * vec[0, :, cols][None] + vec[1, :, cols][None]
            lin[pl.ds(r * 64, 64), cols] = v.reshape(64, 128).astype(BF16)

    def project(b, lin, next_b, next_lin):
        def turned(v, t):
            at = pl.ds(b * ROWS, ROWS)
            inv = lax.rsqrt(jnp.mean(v * v, axis=-1, keepdims=True) + NORM_EPSILON)
            return ((v * tab[t, at, :] + swap_quarters(v) * tab[t + 1, at, :]) * inv).astype(BF16)

        for n in (2, 0, 1):
            out = jnp.dot(lin[...], wqkv[:, pl.ds(n * 256, 256)], preferred_element_type=F32)
            if next_b is not None:
                for r in {2: (0, 1), 0: (2, 3), 1: ()}[n]:
                    modulate(next_b, next_lin, r)
            first, second = out[:, :128], out[:, 128:]
            if n < 2:
                for h, v in ((2 * n, first), (2 * n + 1, second)):
                    t = turned(v, 0)
                    qb[2 * b, pl.ds(h * 128, 128), :] = t[:128]
                    qb[2 * b + 1, pl.ds(h * 128, 128), :] = t[128:]
            else:
                rows = pl.ds(WINDOW + b * ROWS, ROWS)
                kvb[rows, pl.ds(0, 128)] = turned(first, 2)
                kvb[rows, pl.ds(128, 128)] = second.astype(BF16)

    for r in range(ROWS // 64):
        modulate(0, lin0, r)
    project(0, lin0, 3, lin1)
    project(3, lin1, 1, lin2)
    first_keys, last_keys = kvb.at[pl.ds(WINDOW, WINDOW), :], kvb.at[pl.ds(TOK, WINDOW), :]
    remote(first_keys, kvb.at[pl.ds(TOK + WINDOW, WINDOW), :], h_s, h_r.at[0], left).start()
    remote(last_keys, kvb.at[pl.ds(0, WINDOW), :], h_s, h_r.at[1], right).start()
    pass_context(True)
    arrived(wo.at[pl.ds(0, 256), :], w_r.at[0])
    for k in range(2):
        rows = wo_rows(blocks[k], quarter, 64 * k, 64)
        remote(rows, rows, w_s, w_r.at[1], x_peer((1, 3)[k])).start()
    for n in range(2):
        to_side(n, 2)
        to_side(n, 3)
        to_partner(n, quarter)
    project(1, lin2, 2, lin3)
    project(2, lin3, None, None)
    pass_context(False)
    for n in range(2):
        to_side(n, 0)
        to_side(n, 1)

    arrived(kvb.at[pl.ds(TOK + WINDOW, WINDOW), :], h_r.at[0])
    arrived(kvb.at[pl.ds(0, WINDOW), :], h_r.at[1])
    stacked = GROUP * WINDOW
    q_row = lax.rem(lax.broadcasted_iota(jnp.int32, (stacked, WINDOW), 0), WINDOW)
    k_row = lax.broadcasted_iota(jnp.int32, (stacked, WINDOW), 1)
    ahead = k_row - q_row

    def window(b):
        rows = pl.ds(pl.multiple_of(b * WINDOW, WINDOW), 3 * WINDOW)
        k = kvb[rows, pl.ds(0, 128)]
        v = kvb[rows, pl.ds(128, 128)]
        s = lax.dot_general(qb[b], k, (((1,), (1,)), ((), ())), preferred_element_type=F32)
        e = jnp.exp2(s)
        no_left = jnp.logical_and(sp == 0, b == 0).astype(jnp.int32) * (2 * WINDOW)
        no_right = jnp.logical_and(sp == n_sp - 1, b == NBLK - 1).astype(jnp.int32) * (2 * WINDOW)
        e_left = jnp.where(ahead >= no_left, e[:, :WINDOW], 0.0)
        e_right = jnp.where(ahead <= -no_right, e[:, 2 * WINDOW :], 0.0)
        p = jnp.concatenate([e_left, e[:, WINDOW : 2 * WINDOW], e_right], axis=1).astype(BF16)
        v2 = jnp.concatenate([v, jnp.ones((3 * WINDOW, 128), BF16)], axis=1)
        return jnp.dot(p, v2, preferred_element_type=F32)

    def window_pair(i, carry):
        b0 = 2 * i + 1
        b1 = lax.rem(2 * i + 2, NBLK)
        o0, o1 = window(b0), window(b1)
        acc[b0] = o0
        acc[b1] = o1
        return carry

    lax.fori_loop(0, NBLK // 2, window_pair, 0)

    arrived(ckv.at[pl.ds(zrows, 3 * zrows), :], c_r.at[2])

    def context_part(b):
        k = ckv[:, pl.ds(0, 128)]
        v = ckv[:, pl.ds(128, 128)]
        s = lax.dot_general(qb[b], k, (((1,), (1,)), ((), ())), preferred_element_type=F32)
        p = jnp.exp2(s).astype(BF16)
        v2 = jnp.concatenate([v, jnp.ones((CTX, 128), BF16)], axis=1)
        return acc[b] + jnp.dot(p, v2, preferred_element_type=F32)

    def finish(o, h):
        at = slice(h * WINDOW, (h + 1) * WINDOW)
        sink_exp = jnp.broadcast_to(jnp.exp(sink[:, h : h + 1]), (WINDOW, 128))
        return (o[at, :128] / (o[at, 128:] + sink_exp)).astype(BF16)

    def pair(members):
        outs = [context_part(2 * lax.rem(tp + dist, NX) + half) for dist, half in members]
        for (dist, half), o in zip(members, outs):
            rows = pl.ds(half * WINDOW, WINDOW)
            for h in range(GROUP):
                cols = pl.ds(h * 128, 128)
                if dist == 0:
                    attx[0, rows, cols] = finish(o, h)
                else:
                    att[dist - 1, rows, cols] = finish(o, h)
            if dist:
                k = 1 + half if dist == 2 else 0
                remote(att.at[dist - 1, rows, :], attx.at[dist, rows, :], a_s, a_r.at[k], x_peer(dist)).start()

    pair(((1, 0), (3, 0)))
    arrived(wo.at[pl.ds(0, 128), :], w_r.at[1])
    for k in range(4):
        to_side(2, k)
    to_partner(2, quarter)
    pair(((1, 1), (3, 1)))
    pair(((2, 0), (2, 1)))
    arrived(wo.at[pl.ds(0, 256), :], w_r.at[2])
    for n in range(2):
        to_partner(n, other)
    pair(((0, 0), (0, 1)))

    def piece(dist, block, cols):
        rows = pl.ds(pl.multiple_of(block * COLS, COLS), COLS)
        return jnp.dot(attx[dist], wo[rows, cols], preferred_element_type=F32)

    loaded(own_wo, 12)

    def own_part(n, carry):
        cols = pl.ds(pl.multiple_of(n * 512, 512), 512)
        mix[:, cols] = piece(0, tp, cols)
        return carry

    lax.fori_loop(0, D // 512, own_part, 0)

    arrived(wo.at[pl.ds(0, 128), :], w_r.at[3])
    to_partner(2, other)
    arrived(wo.at[pl.ds(0, 512), :], w_r.at[4])
    arrived(attx.at[pl.ds(0, 2)], a_r.at[0])

    def near_part(n, carry):
        cols = pl.ds(pl.multiple_of(n * 512, 512), 512)
        mix[:, cols] = mix[:, cols] + (piece(1, x_before, cols) + piece(3, x_after, cols))
        return carry

    lax.fori_loop(0, D // 512, near_part, 0)

    arrived(wo.at[pl.ds(0, 256), :], w_r.at[5])

    far_block = pl.ds(pl.multiple_of(x_far * COLS, COLS), COLS)
    for half in range(2):
        rows = pl.ds(half * WINDOW, WINDOW)
        arrived(attx.at[2, rows, :], a_r.at[1 + half])

        def far_part(n, carry):
            cols = pl.ds(pl.multiple_of(n * 512, 512), 512)
            mixed = mix[rows, cols] + jnp.dot(attx[2, rows, :], wo[far_block, cols], preferred_element_type=F32)
            own = lat[pl.ds(pl.multiple_of(tp * SUB + half * WINDOW, WINDOW), WINDOW), cols].astype(F32)
            mixed = mixed.reshape(WINDOW // 8, 8, 512) * vec[4, :, cols][None]
            res[rows, cols] = (own + mixed.reshape(WINDOW, 512)).astype(BF16)
            return carry

        lax.fori_loop(0, D // 512, far_part, 0)
        pltpu.make_async_copy(res.at[rows, :], out_h.at[rows, :], o_s).start()

    left_here(zm, m_s.at[0])
    left_here(jm.at[pl.ds(1, NX * NY - 1)], m_s.at[1])
    left_here(cz, c_s.at[0])
    left_here(ckv.at[pl.ds(0, 6 * near), :], c_s.at[1])
    left_here(kvb.at[pl.ds(0, 2 * WINDOW), :], h_s)
    left_here(att, a_s)
    left_here(wo.at[pl.ds(0, 1536), :], w_s)
    pltpu.make_async_copy(res, out_h, o_s).wait()


def per_device(*args):
    (latent, context, cond, ctx_cond, norm_gain, mod_shift, mod_scale, mod_gate, w_query, w_key, w_value, w_out,
     q_gain, k_gain, sinks) = args
    rows, cols = rope_tables(NY * NZ)
    operands = (
        latent[0], context[0], cond, ctx_cond.reshape(1, D), norm_gain.reshape(1, D), mod_shift, mod_scale,
        mod_gate, w_query, w_key, w_value, w_out, q_gain.reshape(1, HEAD_DIM), k_gain.reshape(1, HEAD_DIM),
        sinks.reshape(1, GROUP), jnp.asarray(rows), jnp.asarray(cols),
    )
    dma = pltpu.SemaphoreType.DMA
    vm = pltpu.VMEM
    scratch = [
        vm((TOK, D), BF16), vm((CROWS, D), BF16), vm((2, D), F32), vm((1, D), F32), vm((3, 64, COLS), BF16),
        vm((D, COLS + 2 * HEAD_DIM), BF16), vm((D, D), BF16), vm((2, HEAD_DIM), F32), vm((1, GROUP), F32),
        vm((2, TOK // GRID_W, HEAD_DIM), F32), vm((2, GRID_W, HEAD_DIM), F32),
        vm((8, COLS), BF16), vm((NZ - 1, 8, COLS), BF16), vm((NX * NY, 8, COLS), BF16), vm((5, 8, D), F32),
        vm((TOK, 128), F32), vm((ROWS, D), BF16), vm((ROWS, D), BF16), vm((ROWS, D), BF16), vm((ROWS, D), BF16),
        vm((CROWS, D), BF16), vm((4, TOK, 128), F32), vm((NBLK, GROUP * WINDOW, 128), BF16),
        vm((TOK + 2 * WINDOW, 256), BF16), vm((CROWS, 256), BF16), vm((NZ - 1, CROWS, 256), BF16), vm((CTX, 256), BF16),
        vm((NBLK, GROUP * WINDOW, 256), F32), vm((NX - 1, SUB, COLS), BF16), vm((NX, SUB, COLS), BF16),
        vm((SUB, D), F32), vm((SUB, D), BF16),
        dma((13,)), dma((2,)), dma((2,)), dma((2,)), dma((3,)), dma, dma((2,)), dma, dma((3,)), dma, dma((6,)), dma,
    ]
    result = pl.pallas_call(
        kernel,
        out_shape=jax.ShapeDtypeStruct((SUB, D), BF16),
        in_specs=[pl.BlockSpec(memory_space=pl.ANY)] * len(operands),
        out_specs=pl.BlockSpec(memory_space=pl.ANY),
        scratch_shapes=scratch,
        compiler_params=pltpu.CompilerParams(
            collective_id=0, has_side_effects=True, vmem_limit_bytes=60 * 1024 * 1024
        ),
    )(*operands)
    return result[None]


def solution(mesh):
    in_specs = (
        P("dp", "sp", None), P("dp", "sp", None), P("dp", None), P(), P(), P("sp", "tp"), P("sp", "tp"),
        P("sp", "tp"), P(None, "tp"), P(None, "tp"), P(None, "tp"), P("tp", None), P(), P(), P("tp"),
    )
    out_specs = P("dp", ("sp", "tp"), None)
    return jax.shard_map(per_device, mesh=mesh, in_specs=in_specs, out_specs=out_specs, check_vma=False)
```
